32 devices in a mesh: grp: 2 (over y), fs: 4 (over z), tp: 4 (over x, core).
Axes of the slice: x: 2, y: 2, z: 4, core: 2. Of those that a mesh axis runs over, the one named last changes fastest.
Arguments:
- layer_input_tokens: bfloat16 [4096, 2048], P(('grp', 'fs')), parts along dimension 0, may hold values from -6 to 6
- attention_norm_gain: float32 [2048], replicated, may hold values from 0.1 to 1.9
- query_projection: bfloat16 [2048, 1024], P('fs', 'tp'), may hold values from -0.125 to 0.125
- key_projection: bfloat16 [2048, 1024], P('fs', 'tp'), may hold values from -0.125 to 0.125
- value_projection: bfloat16 [2048, 2048], P('fs', 'tp'), may hold values from -0.125 to 0.125
- decay_first_factor: bfloat16 [2048, 16], replicated, may hold values from -0.125 to 0.125
- decay_second_factor: bfloat16 [16, 1024], P(None, 'tp'), may hold values from -1.5 to 1.5
- decay_logit_bias: float32 [1024], P('tp'), may hold values from -0.5 to 6
- extra_log_decay: float32 [4096, 8], P(('grp', 'fs'), 'tp'), parts along dimension 0, may hold values from -0.7 to 0
- head_output_gain: float32 [256], replicated, may hold values from 0.1 to 1.9
- attention_output_projection: bfloat16 [2048, 2048], P(('tp', 'fs')), may hold values from -0.125 to 0.125
- feedforward_norm_gain: float32 [2048], replicated, may hold values from 0.1 to 1.9
- gate_projection: bfloat16 [2048, 5632], P('fs', 'tp'), may hold values from -0.125 to 0.125
- up_projection: bfloat16 [2048, 5632], P('fs', 'tp'), may hold values from -0.125 to 0.125
- down_projection: bfloat16 [5632, 2048], P(('tp', 'fs')), may hold values from -0.078125 to 0.078125
Outputs:
- result: bfloat16 [4096, 2048], P(('grp', 'fs')), parts along dimension 0
The draws below stay inside these ranges and needn't reach their ends.
There are 2 independent parts, one for each index of `grp`. The reference program is written for one: setup_inputs(seed, part) draws one part's arguments, and reference() takes and returns one part's arrays. A program takes and returns all parts, laid end to end along the dimension named above; an argument that names none is the same for every part. Nothing has to cross between parts.
All inputs are finite; a program needn't handle non-finite values.
Results may differ from the reference program's by a relative error of at most 0.02.
Values may be sent and summed in bfloat16 or wider, within the bound.
No kernel may reach another device: no remote copies, remote signals or barrier semaphores. Data moves between devices by JAX's collectives and lax.ppermute only.
A program may use at most 64 MiB of HBM per device.

```python
import jax
import jax.numpy as jnp
from jax import lax

D = 2048
HEADS = 8
KEY_CHANNELS = 128
DV = 256
RANK = 16
FF = 5632
BLOCK = 64
SEQ_LEN = 512
TOKENS = 2048
N_FS = 4
N_TP = 4


def draw_decay_logit_bias(key, part):
    pick = jax.random.randint(jax.random.fold_in(key, 11), (HEADS * KEY_CHANNELS,), 0, 10)
    fast = jax.random.uniform(jax.random.fold_in(key, 12), (HEADS * KEY_CHANNELS,), jnp.float32, -0.5, 1.0)
    slow = jax.random.uniform(jax.random.fold_in(key, 13), (HEADS * KEY_CHANNELS,), jnp.float32, 3.5, 5.5)
    return jnp.where(pick < 5, fast, slow).astype(jnp.float32)


def draw_extra_log_decay(key, part):
    hits = jax.random.randint(jax.random.fold_in(key, 21), (TOKENS, HEADS), 0, SEQ_LEN)
    depth = jnp.log(jax.random.uniform(jax.random.fold_in(key, 22), (TOKENS, HEADS), jnp.float32, 0.5, 0.8))
    return jnp.where(hits < 3, depth, 0.0).astype(jnp.float32)


def shard_levels(stream_key, extent, cuts, smallest, largest):
    def one(dim, parts):
        steps = jax.random.uniform(jax.random.fold_in(jax.random.fold_in(stream_key, 6), dim), (parts,), jnp.float32, smallest / len(cuts), largest / len(cuts))
        return jnp.repeat(jnp.exp(steps), extent[dim] // parts).reshape((-1,) + (1,) * (len(extent) - dim - 1))

    level = one(*cuts[0])
    for cut in cuts[1:]:
        level = level * one(*cut)
    return level


def noise(own_key, dims, deviation, most, cuts=(), held_as=jnp.bfloat16):
    entries = deviation * jax.random.normal(own_key, dims, jnp.float32)
    if cuts:
        entries = entries * shard_levels(own_key, dims, cuts, -0.22, 0.18)
    return jnp.clip(entries, -most, most).astype(held_as)


def setup_inputs(seed: int = 0, part: int = 0) -> dict:
    seeds = jax.random.split(jax.random.key(seed), 16)
    part_splits = jax.random.split(jax.random.fold_in(seeds[15], part), 16)
    layer_input_tokens = noise(part_splits[0], (TOKENS, D), 1.0, 6.0, ((0, 4),))
    attention_norm_gain = jnp.clip(1.0 + 0.18 * jax.random.normal(seeds[1], (D,), jnp.float32), 0.1, 1.9)
    query_projection = noise(seeds[2], (D, HEADS * KEY_CHANNELS), D ** -0.5, 0.125, ((0, 4), (1, 4)))
    key_projection = noise(seeds[3], (D, HEADS * KEY_CHANNELS), D ** -0.5, 0.125, ((0, 4), (1, 4)))
    value_projection = noise(seeds[4], (D, HEADS * DV), D ** -0.5, 0.125, ((0, 4), (1, 4)))
    decay_first_factor = noise(seeds[5], (D, RANK), D ** -0.5, 0.125)
    decay_second_factor = noise(seeds[6], (RANK, HEADS * KEY_CHANNELS), RANK ** -0.5, 1.5, ((1, 4),))
    decay_logit_bias = draw_decay_logit_bias(jax.random.fold_in(seeds[15], 71), part)
    extra_log_decay = draw_extra_log_decay(jax.random.fold_in(jax.random.fold_in(seeds[15], part), 71), part)
    head_output_gain = jnp.clip(1.0 + 0.18 * jax.random.normal(seeds[9], (DV,), jnp.float32), 0.1, 1.9)
    attention_output_projection = noise(seeds[10], (HEADS * DV, D), (HEADS * DV) ** -0.5, 0.125, ((0, 16),))
    feedforward_norm_gain = jnp.clip(1.0 + 0.18 * jax.random.normal(seeds[11], (D,), jnp.float32), 0.1, 1.9)
    gate_projection = noise(seeds[12], (D, FF), D ** -0.5, 0.125, ((0, 4), (1, 4)))
    up_projection = noise(seeds[13], (D, FF), D ** -0.5, 0.125, ((0, 4), (1, 4)))
    down_projection = noise(seeds[14], (FF, D), FF ** -0.5, 0.078125, ((0, 16),))
    return {"layer_input_tokens": layer_input_tokens, "attention_norm_gain": attention_norm_gain, "query_projection": query_projection, "key_projection": key_projection, "value_projection": value_projection, "decay_first_factor": decay_first_factor, "decay_second_factor": decay_second_factor, "decay_logit_bias": decay_logit_bias, "extra_log_decay": extra_log_decay, "head_output_gain": head_output_gain, "attention_output_projection": attention_output_projection, "feedforward_norm_gain": feedforward_norm_gain, "gate_projection": gate_projection, "up_projection": up_projection, "down_projection": down_projection}


normed_gate = 16.0

def norm_rows(values, gain):
    wide = values.astype(jnp.float32)
    scale = lax.rsqrt(lax.optimization_barrier(jnp.mean(wide * wide, axis=-1, keepdims=True)) + 1e-06)
    return wide * scale * gain

def block_scan(queries, keys, values, decays):
    length, key_channel_width = queries.shape
    value_width = values.shape[1]
    count = length // BLOCK
    lower_mask = jnp.arange(BLOCK)[:, None] >= jnp.arange(BLOCK)[None, :]

    def advance(carry, items):
        query_block, key_block, value_block, decay_block = items
        running = jnp.cumsum(decay_block, axis=0)
        middle = running[BLOCK // 2 - 1]
        closing = running[BLOCK - 1]
        carried = jnp.dot(query_block * jnp.exp(running), carry, precision=lax.Precision.HIGHEST)
        scores = jnp.dot(query_block * jnp.exp(running - middle), (key_block * jnp.exp(middle - running)).T, precision=lax.Precision.HIGHEST)
        scores = jnp.where(lower_mask, scores, 0.0)
        inside = jnp.dot(scores, value_block, precision=lax.Precision.HIGHEST)
        fresh = carry * jnp.exp(closing)[:, None] + jnp.dot((key_block * jnp.exp(closing - running)).T, value_block, precision=lax.Precision.HIGHEST)
        return (fresh, carried + inside)
    items = (queries.reshape(count, BLOCK, key_channel_width), keys.reshape(count, BLOCK, key_channel_width), values.reshape(count, BLOCK, value_width), decays.reshape(count, BLOCK, key_channel_width))
    _, outputs = lax.scan(advance, jnp.zeros((key_channel_width, value_width), jnp.float32), items)
    return outputs.reshape(length, value_width)

def both_ways(queries, keys, values, decays):
    ahead = block_scan(queries, keys, values, decays)
    behind = block_scan(jnp.flip(queries, 0), jnp.flip(keys, 0), jnp.flip(values, 0), jnp.flip(decays, 0))
    return ahead + jnp.flip(behind, 0)

def head_norm(mixed, gain):
    scale = lax.rsqrt(lax.optimization_barrier(jnp.mean(mixed * mixed, axis=-1, keepdims=True)) + 1e-06)
    return mixed * scale * gain

def group_sum(left, right):
    width = left.shape[1] // N_TP
    total = jnp.zeros((left.shape[0], right.shape[1]), jnp.float32)
    for group in range(N_TP):
        part = jnp.dot(left[:, group * width:(group + 1) * width], right[group * width:(group + 1) * width], preferred_element_type=jnp.float32)
        part = lax.optimization_barrier(part.astype(jnp.bfloat16))
        total = total + part.astype(jnp.float32)
    return total

def reference(layer_input_tokens, attention_norm_gain, query_projection, key_projection, value_projection, decay_first_factor, decay_second_factor, decay_logit_bias, extra_log_decay, head_output_gain, attention_output_projection, feedforward_norm_gain, gate_projection, up_projection, down_projection):
    normed = norm_rows(layer_input_tokens, attention_norm_gain).astype(jnp.bfloat16)
    query = jnp.dot(normed, query_projection, preferred_element_type=jnp.float32).astype(jnp.bfloat16)
    key = jnp.dot(normed, key_projection, preferred_element_type=jnp.float32).astype(jnp.bfloat16)
    value = jnp.dot(normed, value_projection, preferred_element_type=jnp.float32).astype(jnp.bfloat16)
    lowrank = jnp.dot(normed, decay_first_factor, preferred_element_type=jnp.float32).astype(jnp.bfloat16)
    decay_logit_values = jnp.dot(lowrank, decay_second_factor, preferred_element_type=jnp.float32) + decay_logit_bias
    decay_logarithm = jax.nn.log_sigmoid(decay_logit_values) / normed_gate + jnp.repeat(extra_log_decay, KEY_CHANNELS, axis=1)

    def sequences(array, width):
        return array.astype(jnp.float32).reshape(N_FS, SEQ_LEN, HEADS, width)
    mixed = jax.vmap(jax.vmap(both_ways, in_axes=1, out_axes=1))(sequences(query, KEY_CHANNELS), sequences(key, KEY_CHANNELS), sequences(value, DV), sequences(decay_logarithm, KEY_CHANNELS))
    headed = head_norm(mixed.reshape(TOKENS, HEADS, DV), head_output_gain)
    headed = headed.reshape(TOKENS, HEADS * DV).astype(jnp.bfloat16)
    mixer = group_sum(headed, attention_output_projection)
    residual = (layer_input_tokens.astype(jnp.float32) + mixer).astype(jnp.bfloat16)
    second = norm_rows(residual, feedforward_norm_gain).astype(jnp.bfloat16)
    gate = jnp.dot(second, gate_projection, preferred_element_type=jnp.float32)
    up = jnp.dot(second, up_projection, preferred_element_type=jnp.float32)
    hidden = (jax.nn.silu(gate) * up).astype(jnp.bfloat16)
    channel = group_sum(hidden, down_projection)
    return (residual.astype(jnp.float32) + channel).astype(jnp.bfloat16)
```

```python
import jax
import jax.numpy as jnp
from jax import lax
from jax.experimental import pallas as pl
from jax.experimental.pallas import tpu as pltpu
from jax.sharding import PartitionSpec as P

BLOCK = 64
DECAY_DIVISOR = 16.0
CORES = 2


def norm_rows(values, gain):
    wide = values.astype(jnp.float32)
    scale = lax.rsqrt(jnp.mean(wide * wide, axis=-1, keepdims=True) + 1e-06)
    return wide * scale * gain


def attention_body(query_ref, key_ref, value_ref, decay_ref, gain_ref, out_ref, acc_ref, ends_ref, fresh_ref, entry_ref):
    length, width = query_ref.shape
    value_width = value_ref.shape[1]
    count = length // BLOCK
    row = lax.broadcasted_iota(jnp.int32, (BLOCK, BLOCK), 0)
    col = lax.broadcasted_iota(jnp.int32, (BLOCK, BLOCK), 1)
    lower, upper = row >= col, row <= col
    sums = jnp.concatenate([lower.astype(jnp.float32), upper.astype(jnp.float32)], axis=0)
    half = BLOCK // 2
    nt = (((1,), (1,)), ((), ()))
    tn = (((0,), (0,)), ((), ()))

    for block in range(count):
        rows = pl.ds(block * BLOCK, BLOCK)
        decay = decay_ref[rows, :]
        both = jnp.dot(sums, decay, precision=lax.Precision.HIGHEST, preferred_element_type=jnp.float32)
        query = query_ref[rows, :].astype(jnp.float32)
        key = key_ref[rows, :].astype(jnp.float32)
        value = value_ref[rows, :]
        scores = None
        carried = []
        outgoing = []
        for running, middle_at, closing_at, mask in (
            (both[:BLOCK], half - 1, BLOCK - 1, lower),
            (both[BLOCK:], half, 0, upper),
        ):
            middle = running[middle_at : middle_at + 1]
            closing = running[closing_at : closing_at + 1]
            left = (query * jnp.exp(running - middle)).astype(jnp.bfloat16)
            right = (key * jnp.exp(middle - running)).astype(jnp.bfloat16)
            part = lax.dot_general(left, right, nt, preferred_element_type=jnp.float32)
            part = jnp.where(mask, part, 0.0)
            scores = part if scores is None else scores + part
            carried.append((query * jnp.exp(running)).astype(jnp.bfloat16))
            outgoing.append((key * jnp.exp(closing - running)).astype(jnp.bfloat16))
            side = len(carried) - 1
            ends_ref[block, :, side * width : (side + 1) * width] = jnp.exp(closing)
        acc_ref[rows, :] = jnp.dot(scores.astype(jnp.bfloat16), value, preferred_element_type=jnp.float32)
        entry_ref[block, :BLOCK, :] = jnp.concatenate(carried, axis=1)
        fresh_ref[block] = lax.dot_general(
            value, jnp.concatenate(outgoing, axis=1), tn, preferred_element_type=jnp.float32
        )

    state = [jnp.zeros((value_width, width), jnp.float32) for _ in range(2)]
    for step in range(count):
        for side, block in ((0, step), (1, count - 1 - step)):
            lanes = slice(side * width, (side + 1) * width)
            entry_ref[block, BLOCK:, lanes] = state[side].astype(jnp.bfloat16)
            state[side] = state[side] * ends_ref[block, :, lanes] + fresh_ref[block, :, lanes]
    for block in range(count):
        rows = pl.ds(block * BLOCK, BLOCK)
        mixed = acc_ref[rows, :] + lax.dot_general(
            entry_ref[block, :BLOCK, :], entry_ref[block, BLOCK:, :], nt, preferred_element_type=jnp.float32
        )
        scale = lax.rsqrt(jnp.mean(mixed * mixed, axis=-1, keepdims=True) + 1e-06)
        out_ref[rows, :] = (mixed * scale * gain_ref[...]).astype(jnp.bfloat16)


def attention(projected, decays, gain, heads):
    length = projected.shape[0]
    width = decays.shape[1] // heads
    value_width = gain.shape[0]
    count = length // BLOCK
    value_first = 2 * heads * width // value_width
    return pl.pallas_call(
        attention_body,
        grid=(heads,),
        in_specs=[
            pl.BlockSpec((length, width), lambda h: (0, h)),
            pl.BlockSpec((length, width), lambda h: (0, heads + h)),
            pl.BlockSpec((length, value_width), lambda h: (0, value_first + h)),
            pl.BlockSpec((length, width), lambda h: (0, h)),
            pl.BlockSpec((1, value_width), lambda h: (0, 0)),
        ],
        out_specs=pl.BlockSpec((length, value_width), lambda h: (0, h)),
        out_shape=jax.ShapeDtypeStruct((length, heads * value_width), jnp.bfloat16),
        scratch_shapes=[
            pltpu.VMEM((length, value_width), jnp.float32),
            pltpu.VMEM((count, 1, 2 * width), jnp.float32),
            pltpu.VMEM((count, value_width, 2 * width), jnp.float32),
            pltpu.VMEM((count, BLOCK + value_width, 2 * width), jnp.bfloat16),
        ],
        name="attention",
    )(projected, projected, projected, decays, gain.reshape(1, -1))


def after(value, *others):
    return lax.optimization_barrier((value, *others))[0]


def gather_rows(shard, wait_for=()):
    fs, grp = lax.axis_size("fs"), lax.axis_size("grp")
    rows = shard.shape[0]
    if fs != 4 or grp != 2 or rows % 32:
        return lax.all_gather(shard, "fs", axis=0, tiled=True), ()
    half = rows // 2
    here, part = lax.axis_index("fs"), lax.axis_index("grp")
    mine = lax.dynamic_slice_in_dim(shard, part * half, half, 0)
    if wait_for:
        mine = after(mine, *wait_for)

    def shift(value, by):
        return lax.ppermute(value, "fs", [(i, (i + by) % fs) for i in range(fs)])

    ahead = shift(mine, 1)
    behind = shift(mine, fs - 1)
    far = shift(ahead, 1)
    full = jnp.zeros((fs * rows, shard.shape[1]), shard.dtype)
    full = lax.dynamic_update_slice_in_dim(full, shard, here * rows, 0)
    for piece, by in ((ahead, 1), (behind, fs - 1), (far, 2)):
        base = ((here + fs - by) % fs) * rows
        other = lax.ppermute(piece, "grp", [(0, 1), (1, 0)])
        full = lax.dynamic_update_slice_in_dim(full, piece, base + part * half, 0)
        full = lax.dynamic_update_slice_in_dim(full, other, base + (1 - part) * half, 0)
    return full, (ahead, behind)


def core_swap(value):
    size = lax.axis_size("tp")
    return lax.ppermute(value, "tp", [(i, i ^ 1) for i in range(size)])


def chip_swap(value):
    size = lax.axis_size("tp")
    return lax.ppermute(value, "tp", [(i, (i + CORES) % size) for i in range(size)])


def small_tp():
    return lax.axis_size("tp") == 2 * CORES


def share_rows(rows):
    if small_tp():
        share = rows // CORES
        return (lax.axis_index("tp") % CORES) * share, share
    share = rows // lax.axis_size("tp")
    return lax.axis_index("tp") * share, share


def sum_groups(part):
    if not small_tp():
        return lax.psum_scatter(part, "tp", scatter_dimension=0, tiled=True).astype(jnp.float32)
    first, share = share_rows(part.shape[0])
    kept = lax.dynamic_slice_in_dim(part, first, share, 0)
    given = lax.dynamic_slice_in_dim(part, share - first, share, 0)
    chip = kept.astype(jnp.float32) + core_swap(given).astype(jnp.float32)
    chip = lax.reduce_precision(chip, 8, 7).astype(jnp.bfloat16)
    chip = lax.optimization_barrier(chip)
    return chip.astype(jnp.float32) + chip_swap(chip).astype(jnp.float32)


def collect_rows(value):
    if not small_tp():
        return lax.all_gather(value, "tp", axis=0, tiled=True)
    share = value.shape[0]
    first = (lax.axis_index("tp") % CORES) * share
    full = jnp.zeros((CORES * share, value.shape[1]), value.dtype)
    full = lax.dynamic_update_slice_in_dim(full, value, first, 0)
    return lax.dynamic_update_slice_in_dim(full, core_swap(value), share - first, 0)


def shards(
    layer_input_tokens,
    attention_norm_gain,
    query_projection,
    key_projection,
    value_projection,
    decay_first_factor,
    decay_second_factor,
    decay_logit_bias,
    extra_log_decay,
    head_output_gain,
    attention_output_projection,
    feedforward_norm_gain,
    gate_projection,
    up_projection,
    down_projection,
):
    rows = layer_input_tokens.shape[0]
    wide = jnp.float32
    local_heads = extra_log_decay.shape[1]
    width = query_projection.shape[1] // local_heads

    packed = jnp.concatenate([query_projection, key_projection, value_projection], axis=1)
    packed_full, first_wave = gather_rows(packed)
    out_full, second_wave = gather_rows(attention_output_projection, first_wave)
    gate_full, gate_wave = gather_rows(gate_projection, second_wave)
    up_full, up_wave = gather_rows(up_projection, gate_wave)
    down_full, _ = gather_rows(down_projection, up_wave)

    normed = norm_rows(layer_input_tokens, attention_norm_gain).astype(jnp.bfloat16)
    lowrank = jnp.dot(normed, decay_first_factor, preferred_element_type=wide).astype(jnp.bfloat16)
    logits = jnp.dot(lowrank, decay_second_factor, preferred_element_type=wide) + decay_logit_bias
    decays = jax.nn.log_sigmoid(logits) / DECAY_DIVISOR + jnp.repeat(extra_log_decay, width, axis=1)

    projected = jnp.dot(normed, packed_full, preferred_element_type=wide).astype(jnp.bfloat16)
    headed = attention(projected, decays, head_output_gain, local_heads)
    mixer = sum_groups(jnp.dot(headed, out_full, preferred_element_type=wide).astype(jnp.bfloat16))

    first, share = share_rows(rows)
    own = lax.dynamic_slice_in_dim(layer_input_tokens, first, share, 0)
    residual = (own.astype(wide) + mixer).astype(jnp.bfloat16)
    second = collect_rows(norm_rows(residual, feedforward_norm_gain).astype(jnp.bfloat16))

    gate = jnp.dot(second, gate_full, preferred_element_type=wide)
    up = jnp.dot(second, up_full, preferred_element_type=wide)
    hidden = (jax.nn.silu(gate) * up).astype(jnp.bfloat16)
    channel = sum_groups(jnp.dot(hidden, down_full, preferred_element_type=wide).astype(jnp.bfloat16))
    finished = (residual.astype(wide) + channel).astype(jnp.bfloat16)
    return collect_rows(finished)


def solution(mesh):
    placed = (
        P(("grp", "fs"), None),
        P(),
        P("fs", "tp"),
        P("fs", "tp"),
        P("fs", "tp"),
        P(),
        P(None, "tp"),
        P("tp"),
        P(("grp", "fs"), "tp"),
        P(),
        P(("tp", "fs"), None),
        P(),
        P("fs", "tp"),
        P("fs", "tp"),
        P(("tp", "fs"), None),
    )
    return jax.shard_map(
        shards, mesh=mesh, in_specs=placed, out_specs=P(("grp", "fs"), None), check_vma=False
    )
```

```python
import jax
import jax.numpy as jnp
from jax import lax
from jax.experimental import pallas as pl
from jax.experimental.pallas import tpu as pltpu
from jax.sharding import PartitionSpec as P


BLOCK = 64
GATE_CUTS = ()
DOWN_CUTS = (0.4, 0.75)
ALONE = (2,)
DECAY_DIVISOR = 16.0
CORES = 2


def norm_rows(values, gain):
    wide = values.astype(jnp.float32)
    scale = lax.rsqrt(jnp.mean(wide * wide, axis=-1, keepdims=True) + 1e-06)
    return wide * scale * gain


def attention_body(query_ref, key_ref, value_ref, decay_ref, gain_ref, out_ref, acc_ref, ends_ref, fresh_ref, entry_ref):
    length, width = query_ref.shape
    value_width = value_ref.shape[1]
    count = length // BLOCK
    row = lax.broadcasted_iota(jnp.int32, (BLOCK, BLOCK), 0)
    col = lax.broadcasted_iota(jnp.int32, (BLOCK, BLOCK), 1)
    lower, upper = row >= col, row <= col
    sums = jnp.concatenate([lower.astype(jnp.float32), upper.astype(jnp.float32)], axis=0)
    half = BLOCK // 2
    nt = (((1,), (1,)), ((), ()))
    tn = (((0,), (0,)), ((), ()))

    for block in range(count):
        rows = pl.ds(block * BLOCK, BLOCK)
        decay = decay_ref[rows, :]
        both = jnp.dot(sums, decay, precision=lax.Precision.HIGHEST, preferred_element_type=jnp.float32)
        query = query_ref[rows, :].astype(jnp.float32)
        key = key_ref[rows, :].astype(jnp.float32)
        value = value_ref[rows, :]
        scores = None
        carried = []
        outgoing = []
        for running, middle_at, closing_at, mask in (
            (both[:BLOCK], half - 1, BLOCK - 1, lower),
            (both[BLOCK:], half, 0, upper),
        ):
            middle = running[middle_at : middle_at + 1]
            closing = running[closing_at : closing_at + 1]
            left = (query * jnp.exp(running - middle)).astype(jnp.bfloat16)
            right = (key * jnp.exp(middle - running)).astype(jnp.bfloat16)
            part = lax.dot_general(left, right, nt, preferred_element_type=jnp.float32)
            part = jnp.where(mask, part, 0.0)
            scores = part if scores is None else scores + part
            carried.append((query * jnp.exp(running)).astype(jnp.bfloat16))
            outgoing.append((key * jnp.exp(closing - running)).astype(jnp.bfloat16))
            side = len(carried) - 1
            ends_ref[block, :, side * width : (side + 1) * width] = jnp.exp(closing)
        acc_ref[rows, :] = jnp.dot(scores.astype(jnp.bfloat16), value, preferred_element_type=jnp.float32)
        entry_ref[block, :BLOCK, :] = jnp.concatenate(carried, axis=1)
        fresh_ref[block] = lax.dot_general(
            value, jnp.concatenate(outgoing, axis=1), tn, preferred_element_type=jnp.float32
        )

    state = [jnp.zeros((value_width, width), jnp.float32) for _ in range(2)]
    for step in range(count):
        for side, block in ((0, step), (1, count - 1 - step)):
            lanes = slice(side * width, (side + 1) * width)
            entry_ref[block, BLOCK:, lanes] = state[side].astype(jnp.bfloat16)
            state[side] = state[side] * ends_ref[block, :, lanes] + fresh_ref[block, :, lanes]
    for block in range(count):
        rows = pl.ds(block * BLOCK, BLOCK)
        mixed = acc_ref[rows, :] + lax.dot_general(
            entry_ref[block, :BLOCK, :], entry_ref[block, BLOCK:, :], nt, preferred_element_type=jnp.float32
        )
        scale = lax.rsqrt(jnp.mean(mixed * mixed, axis=-1, keepdims=True) + 1e-06)
        out_ref[rows, :] = (mixed * scale * gain_ref[...]).astype(jnp.bfloat16)


def attention(projected, decays, gain, heads):
    length = projected.shape[0]
    width = decays.shape[1] // heads
    value_width = gain.shape[0]
    count = length // BLOCK
    value_first = 2 * heads * width // value_width
    return pl.pallas_call(
        attention_body,
        grid=(heads,),
        in_specs=[
            pl.BlockSpec((length, width), lambda h: (0, h)),
            pl.BlockSpec((length, width), lambda h: (0, heads + h)),
            pl.BlockSpec((length, value_width), lambda h: (0, value_first + h)),
            pl.BlockSpec((length, width), lambda h: (0, h)),
            pl.BlockSpec((1, value_width), lambda h: (0, 0)),
        ],
        out_specs=pl.BlockSpec((length, value_width), lambda h: (0, h)),
        out_shape=jax.ShapeDtypeStruct((length, heads * value_width), jnp.bfloat16),
        scratch_shapes=[
            pltpu.VMEM((length, value_width), jnp.float32),
            pltpu.VMEM((count, 1, 2 * width), jnp.float32),
            pltpu.VMEM((count, value_width, 2 * width), jnp.float32),
            pltpu.VMEM((count, BLOCK + value_width, 2 * width), jnp.bfloat16),
        ],
        name="attention",
    )(projected, projected, projected, decays, gain.reshape(1, -1))


def gather_columns(parts):
    return parts[0] if len(parts) == 1 else jnp.concatenate(parts, axis=1)


def by_permutes(shape, rows):
    return shape["fs"] == 4 and shape["grp"] == 2 and rows % 32 == 0


def gather_rows(parts, alone=False):
    fs, grp = lax.axis_size("fs"), lax.axis_size("grp")
    rows = parts[0].shape[0]
    if not by_permutes({"fs": fs, "grp": grp}, rows):
        return [lax.all_gather(gather_columns(parts), "fs", axis=0, tiled=True)], [jnp.int32(0)]
    here, part = lax.axis_index("fs"), lax.axis_index("grp")
    shard = gather_columns(parts)
    half = rows if alone else rows // 2
    mine = shard
    if not alone:
        mine = gather_columns([lax.dynamic_slice_in_dim(p, part * half, half, 0) for p in parts])

    def shift(value, by):
        return lax.ppermute(value, "fs", [(i, (i + by) % fs) for i in range(fs)])

    def swap(value):
        return lax.ppermute(value, "grp", [(0, 1), (1, 0)])

    ahead = shift(mine, 1)
    behind = shift(mine, fs - 1)
    far = shift(ahead, 1)
    pieces, firsts = [shard], [here * rows]
    for piece, by in ((ahead, 1), (behind, fs - 1), (far, 2)):
        base = ((here + fs - by) % fs) * rows
        if alone:
            pieces.append(piece)
            firsts.append(base)
        else:
            pieces += [piece, swap(piece)]
            firsts += [base + part * half, base + (1 - part) * half]
    return pieces, firsts


def join(firsts, refs, full_ref, unit):
    for index, ref in enumerate(refs):
        first = pl.multiple_of(firsts[index], unit)
        full_ref[pl.ds(first, ref.shape[0]), :] = ref[...]


def pieces_unit(pieces):
    unit = 1
    while all(p.shape[0] % (2 * unit) == 0 for p in pieces):
        unit *= 2
    return unit


def dot_pieces(blocks, gathered, tile=256):
    pieces, firsts = gathered
    rows, columns = blocks[0].shape[0], pieces[0].shape[1]
    depth = sum(b.shape[1] for b in blocks)
    tile = min(tile, columns)
    unit = pieces_unit(pieces)

    def body(firsts_ref, *refs):
        left = refs[: len(blocks)]
        out_ref, full_ref, left_ref = refs[-3:]

        @pl.when(pl.program_id(0) == 0)
        def _():
            at = 0
            for ref in left:
                left_ref[:, at : at + ref.shape[1]] = ref[...]
                at += ref.shape[1]

        join([firsts_ref[i] for i in range(len(pieces))], refs[len(blocks) : -3], full_ref, unit)
        out_ref[...] = jnp.dot(left_ref[...], full_ref[...], preferred_element_type=jnp.float32).astype(jnp.bfloat16)

    return pl.pallas_call(
        body,
        grid=(pl.cdiv(columns, tile),),
        in_specs=[pl.BlockSpec(memory_space=pltpu.SMEM)]
        + [pl.BlockSpec(b.shape, lambda i: (0, 0)) for b in blocks]
        + [pl.BlockSpec((p.shape[0], tile), lambda i: (0, i)) for p in pieces],
        out_specs=pl.BlockSpec((rows, tile), lambda i: (0, i)),
        out_shape=jax.ShapeDtypeStruct((rows, columns), jnp.bfloat16),
        scratch_shapes=[pltpu.VMEM((depth, tile), jnp.bfloat16), pltpu.VMEM((rows, depth), jnp.bfloat16)],
    )(jnp.stack(firsts).astype(jnp.int32), *blocks, *pieces)


def gated(halves, gate, up, tile=256):
    rows_pieces, row_firsts = halves
    gate_pieces, firsts = gate
    up_pieces = up[0]
    rows = sum(h.shape[0] for h in rows_pieces)
    depth, units = rows_pieces[0].shape[1], gate_pieces[0].shape[1]
    count, parts = len(gate_pieces), len(rows_pieces)
    unit, row_unit = pieces_unit(gate_pieces), pieces_unit(rows_pieces)

    def body(firsts_ref, *refs):
        out_ref, gate_ref, up_ref, second_ref = refs[-4:]

        @pl.when(pl.program_id(0) == 0)
        def _():
            join([firsts_ref[count + i] for i in range(parts)], refs[:parts], second_ref, row_unit)

        where = [firsts_ref[i] for i in range(count)]
        join(where, refs[parts : parts + count], gate_ref, unit)
        join(where, refs[parts + count : -4], up_ref, unit)
        second = second_ref[...]
        gate_sum = jnp.dot(second, gate_ref[...], preferred_element_type=jnp.float32)
        up_sum = jnp.dot(second, up_ref[...], preferred_element_type=jnp.float32)
        out_ref[...] = (gate_sum / (1.0 + jnp.exp(-gate_sum)) * up_sum).astype(jnp.bfloat16)

    return pl.pallas_call(
        body,
        grid=(pl.cdiv(units, tile),),
        in_specs=[pl.BlockSpec(memory_space=pltpu.SMEM)]
        + [pl.BlockSpec(h.shape, lambda i: (0, 0)) for h in rows_pieces]
        + [pl.BlockSpec((p.shape[0], tile), lambda i: (0, i)) for p in gate_pieces + up_pieces],
        out_specs=pl.BlockSpec((rows, tile), lambda i: (0, i)),
        out_shape=jax.ShapeDtypeStruct((rows, units), jnp.bfloat16),
        scratch_shapes=[
            pltpu.VMEM((depth, tile), jnp.bfloat16),
            pltpu.VMEM((depth, tile), jnp.bfloat16),
            pltpu.VMEM((rows, depth), jnp.bfloat16),
        ],
    )(jnp.stack(firsts + row_firsts).astype(jnp.int32), *rows_pieces, *gate_pieces, *up_pieces)


def blank_body(out_ref):
    pass


def blank(shape, dtype):
    return pl.pallas_call(
        blank_body,
        out_specs=pl.BlockSpec(memory_space=pl.ANY),
        out_shape=jax.ShapeDtypeStruct(shape, dtype),
        name="blank",
    )()


def core_swap(value):
    size = lax.axis_size("tp")
    return lax.ppermute(value, "tp", [(i, i ^ 1) for i in range(size)])


def chip_swap(value):
    size = lax.axis_size("tp")
    return lax.ppermute(value, "tp", [(i, (i + CORES) % size) for i in range(size)])


def small_tp():
    return lax.axis_size("tp") == 2 * CORES


def share_rows(rows):
    if small_tp():
        share = rows // CORES
        return (lax.axis_index("tp") % CORES) * share, share
    share = rows // lax.axis_size("tp")
    return lax.axis_index("tp") * share, share


def sum_groups(part):
    if not small_tp():
        return lax.psum_scatter(part, "tp", scatter_dimension=0, tiled=True).astype(jnp.float32)
    first, share = share_rows(part.shape[0])
    kept = lax.dynamic_slice_in_dim(part, first, share, 0)
    given = lax.dynamic_slice_in_dim(part, share - first, share, 0)
    chip = kept.astype(jnp.float32) + core_swap(given).astype(jnp.float32)
    chip = lax.reduce_precision(chip, 8, 7).astype(jnp.bfloat16)
    chip = lax.optimization_barrier(chip)
    return chip.astype(jnp.float32) + chip_swap(chip).astype(jnp.float32)


def collect_rows(value):
    if not small_tp():
        return [lax.all_gather(value, "tp", axis=0, tiled=True)], [jnp.int32(0)]
    share = value.shape[0]
    first = (lax.axis_index("tp") % CORES) * share
    return [value, core_swap(value)], [first, share - first]


def shards(
    layer_input_tokens,
    attention_norm_gain,
    query_projection,
    key_projection,
    value_projection,
    decay_first_factor,
    decay_second_factor,
    decay_logit_bias,
    extra_log_decay,
    head_output_gain,
    attention_output_projection,
    feedforward_norm_gain,
    gate_projection,
    up_projection,
    down_projection,
):
    rows = layer_input_tokens.shape[0]
    wide = jnp.float32
    local_heads = extra_log_decay.shape[1]
    width = query_projection.shape[1] // local_heads

    out_pieces = gather_rows([attention_output_projection])
    packed_pieces = gather_rows([query_projection, key_projection, value_projection])
    gates = [gather_rows([gate_projection[:, a:b]]) for a, b in spans(gate_projection, GATE_CUTS)]
    ups = [gather_rows([up_projection[:, a:b]]) for a, b in spans(up_projection, GATE_CUTS)]
    down_spans = spans(down_projection, DOWN_CUTS)
    downs = [gather_rows([down_projection[:, a:b]], alone=i in ALONE) for i, (a, b) in enumerate(down_spans)]

    normed = norm_rows(layer_input_tokens, attention_norm_gain).astype(jnp.bfloat16)
    lowrank = jnp.dot(normed, decay_first_factor, preferred_element_type=wide).astype(jnp.bfloat16)
    logits = jnp.dot(lowrank, decay_second_factor, preferred_element_type=wide) + decay_logit_bias
    decays = jax.nn.log_sigmoid(logits) / DECAY_DIVISOR + jnp.repeat(extra_log_decay, width, axis=1)

    projected = dot_pieces([normed], packed_pieces)
    headed = attention(projected, decays, head_output_gain, local_heads)
    mixer = sum_groups(dot_pieces([headed], out_pieces, 512))

    first, share = share_rows(rows)
    own = lax.dynamic_slice_in_dim(layer_input_tokens, first, share, 0)
    residual = (own.astype(wide) + mixer).astype(jnp.bfloat16)
    second = collect_rows(norm_rows(residual, feedforward_norm_gain).astype(jnp.bfloat16))

    hidden = [gated(second, gates[i], ups[i]) for i in range(len(gates))]
    result = blank(layer_input_tokens.shape, jnp.bfloat16)
    for chunk, (start, stop) in enumerate(down_spans):
        channel = sum_groups(dot_pieces(hidden, downs[chunk]))
        finished = (residual[:, start:stop].astype(wide) + channel).astype(jnp.bfloat16)
        for piece, at in zip(*collect_rows(finished)):
            result = lax.dynamic_update_slice(result, piece, (at, jnp.int32(start)))
    return result


def spans(weight, cuts):
    width = weight.shape[1]
    edges = [0] + [round(width * cut / 128) * 128 for cut in cuts] + [width]
    return list(zip(edges, edges[1:]))


def solution(mesh):
    placed = (
        P(("grp", "fs"), None),
        P(),
        P("fs", "tp"),
        P("fs", "tp"),
        P("fs", "tp"),
        P(),
        P(None, "tp"),
        P("tp"),
        P(("grp", "fs"), "tp"),
        P(),
        P(("tp", "fs"), None),
        P(),
        P("fs", "tp"),
        P("fs", "tp"),
        P(("tp", "fs"), None),
    )

    return jax.shard_map(shards, mesh=mesh, in_specs=placed, out_specs=P(("grp", "fs"), None), check_vma=False)
```

```python
import jax
import jax.numpy as jnp
from jax import lax
from jax.experimental import pallas as pl
from jax.experimental.pallas import tpu as pltpu
from jax.sharding import PartitionSpec as P


BLOCK = 64
GATE_CUTS = ()
DOWN_CUTS = (0.5, 0.75)
ALONE = (1, 2)
DECAY_DIVISOR = 16.0
CORES = 2


def norm_rows(values, gain):
    wide = values.astype(jnp.float32)
    scale = lax.rsqrt(jnp.mean(wide * wide, axis=-1, keepdims=True) + 1e-06)
    return wide * scale * gain


def attention_body(query_ref, key_ref, value_ref, decay_ref, gain_ref, out_ref, acc_ref, ends_ref, fresh_ref, entry_ref):
    length, width = query_ref.shape
    value_width = value_ref.shape[1]
    count = length // BLOCK
    row = lax.broadcasted_iota(jnp.int32, (BLOCK, BLOCK), 0)
    col = lax.broadcasted_iota(jnp.int32, (BLOCK, BLOCK), 1)
    lower, upper = row >= col, row <= col
    sums = jnp.concatenate([lower.astype(jnp.float32), upper.astype(jnp.float32)], axis=0)
    half = BLOCK // 2
    nt = (((1,), (1,)), ((), ()))
    tn = (((0,), (0,)), ((), ()))

    for block in range(count):
        rows = pl.ds(block * BLOCK, BLOCK)
        decay = decay_ref[rows, :]
        both = jnp.dot(sums, decay, precision=lax.Precision.HIGHEST, preferred_element_type=jnp.float32)
        query = query_ref[rows, :].astype(jnp.float32)
        key = key_ref[rows, :].astype(jnp.float32)
        value = value_ref[rows, :]
        scores = None
        carried = []
        outgoing = []
        for running, middle_at, closing_at, mask in (
            (both[:BLOCK], half - 1, BLOCK - 1, lower),
            (both[BLOCK:], half, 0, upper),
        ):
            middle = running[middle_at : middle_at + 1]
            closing = running[closing_at : closing_at + 1]
            left = (query * jnp.exp(running - middle)).astype(jnp.bfloat16)
            right = (key * jnp.exp(middle - running)).astype(jnp.bfloat16)
            part = lax.dot_general(left, right, nt, preferred_element_type=jnp.float32)
            part = jnp.where(mask, part, 0.0)
            scores = part if scores is None else scores + part
            carried.append((query * jnp.exp(running)).astype(jnp.bfloat16))
            outgoing.append((key * jnp.exp(closing - running)).astype(jnp.bfloat16))
            side = len(carried) - 1
            ends_ref[block, :, side * width : (side + 1) * width] = jnp.exp(closing)
        acc_ref[rows, :] = jnp.dot(scores.astype(jnp.bfloat16), value, preferred_element_type=jnp.float32)
        entry_ref[block, :BLOCK, :] = jnp.concatenate(carried, axis=1)
        fresh_ref[block] = lax.dot_general(
            value, jnp.concatenate(outgoing, axis=1), tn, preferred_element_type=jnp.float32
        )

    state = [jnp.zeros((value_width, width), jnp.float32) for _ in range(2)]
    for step in range(count):
        for side, block in ((0, step), (1, count - 1 - step)):
            lanes = slice(side * width, (side + 1) * width)
            entry_ref[block, BLOCK:, lanes] = state[side].astype(jnp.bfloat16)
            state[side] = state[side] * ends_ref[block, :, lanes] + fresh_ref[block, :, lanes]
    for block in range(count):
        rows = pl.ds(block * BLOCK, BLOCK)
        mixed = acc_ref[rows, :] + lax.dot_general(
            entry_ref[block, :BLOCK, :], entry_ref[block, BLOCK:, :], nt, preferred_element_type=jnp.float32
        )
        scale = lax.rsqrt(jnp.mean(mixed * mixed, axis=-1, keepdims=True) + 1e-06)
        out_ref[rows, :] = (mixed * scale * gain_ref[...]).astype(jnp.bfloat16)


def attention(projected, decays, gain, heads):
    length = projected.shape[0]
    width = decays.shape[1] // heads
    value_width = gain.shape[0]
    count = length // BLOCK
    value_first = 2 * heads * width // value_width
    return pl.pallas_call(
        attention_body,
        grid=(heads,),
        in_specs=[
            pl.BlockSpec((length, width), lambda h: (0, h)),
            pl.BlockSpec((length, width), lambda h: (0, heads + h)),
            pl.BlockSpec((length, value_width), lambda h: (0, value_first + h)),
            pl.BlockSpec((length, width), lambda h: (0, h)),
            pl.BlockSpec((1, value_width), lambda h: (0, 0)),
        ],
        out_specs=pl.BlockSpec((length, value_width), lambda h: (0, h)),
        out_shape=jax.ShapeDtypeStruct((length, heads * value_width), jnp.bfloat16),
        scratch_shapes=[
            pltpu.VMEM((length, value_width), jnp.float32),
            pltpu.VMEM((count, 1, 2 * width), jnp.float32),
            pltpu.VMEM((count, value_width, 2 * width), jnp.float32),
            pltpu.VMEM((count, BLOCK + value_width, 2 * width), jnp.bfloat16),
        ],
        name="attention",
    )(projected, projected, projected, decays, gain.reshape(1, -1))


def gather_columns(parts):
    return parts[0] if len(parts) == 1 else jnp.concatenate(parts, axis=1)


def by_permutes(shape, rows):
    return shape["fs"] == 4 and shape["grp"] == 2 and rows % 32 == 0


def gather_rows(parts, alone=False, early=None):
    fs, grp = lax.axis_size("fs"), lax.axis_size("grp")
    rows = parts[0].shape[0]
    if not by_permutes({"fs": fs, "grp": grp}, rows):
        return [lax.all_gather(gather_columns(parts), "fs", axis=0, tiled=True)], [jnp.int32(0)]
    here, part = lax.axis_index("fs"), lax.axis_index("grp")
    shard = gather_columns(parts)
    half = rows if alone else rows // 2
    mine = shard
    if not alone:
        mine = gather_columns([lax.dynamic_slice_in_dim(p, part * half, half, 0) for p in parts])

    def shift(value, by):
        return lax.ppermute(value, "fs", [(i, (i + by) % fs) for i in range(fs)])

    def swap(value):
        return lax.ppermute(value, "grp", [(0, 1), (1, 0)])

    ahead = shift(mine, 1)
    behind = shift(mine, fs - 1)
    far = shift(ahead, 1)
    if early is not None:
        far = lax.optimization_barrier((far, early))[0]
    pieces, firsts = [shard], [here * rows]
    for piece, by in ((ahead, 1), (behind, fs - 1), (far, 2)):
        base = ((here + fs - by) % fs) * rows
        if alone:
            pieces.append(piece)
            firsts.append(base)
        else:
            pieces += [piece, swap(piece)]
            firsts += [base + part * half, base + (1 - part) * half]
    return pieces, firsts


def join(firsts, refs, full_ref, unit):
    for index, ref in enumerate(refs):
        first = pl.multiple_of(firsts[index], unit)
        full_ref[pl.ds(first, ref.shape[0]), :] = ref[...]


def pieces_unit(pieces):
    unit = 1
    while all(p.shape[0] % (2 * unit) == 0 for p in pieces):
        unit *= 2
    return unit


def dot_pieces(blocks, gathered, tile=256):
    pieces, firsts = gathered
    rows, columns = blocks[0].shape[0], pieces[0].shape[1]
    depth = sum(b.shape[1] for b in blocks)
    tile = min(tile, columns)
    unit = pieces_unit(pieces)

    def body(firsts_ref, *refs):
        left = refs[: len(blocks)]
        out_ref, full_ref, left_ref = refs[-3:]

        @pl.when(pl.program_id(0) == 0)
        def _():
            at = 0
            for ref in left:
                left_ref[:, at : at + ref.shape[1]] = ref[...]
                at += ref.shape[1]

        join([firsts_ref[i] for i in range(len(pieces))], refs[len(blocks) : -3], full_ref, unit)
        out_ref[...] = jnp.dot(left_ref[...], full_ref[...], preferred_element_type=jnp.float32).astype(jnp.bfloat16)

    return pl.pallas_call(
        body,
        grid=(pl.cdiv(columns, tile),),
        in_specs=[pl.BlockSpec(memory_space=pltpu.SMEM)]
        + [pl.BlockSpec(b.shape, lambda i: (0, 0)) for b in blocks]
        + [pl.BlockSpec((p.shape[0], tile), lambda i: (0, i)) for p in pieces],
        out_specs=pl.BlockSpec((rows, tile), lambda i: (0, i)),
        out_shape=jax.ShapeDtypeStruct((rows, columns), jnp.bfloat16),
        scratch_shapes=[pltpu.VMEM((depth, tile), jnp.bfloat16), pltpu.VMEM((rows, depth), jnp.bfloat16)],
    )(jnp.stack(firsts).astype(jnp.int32), *blocks, *pieces)


def gated(halves, gate, up, tile=256):
    rows_pieces, row_firsts = halves
    gate_pieces, firsts = gate
    up_pieces = up[0]
    rows = sum(h.shape[0] for h in rows_pieces)
    depth, units = rows_pieces[0].shape[1], gate_pieces[0].shape[1]
    count, parts = len(gate_pieces), len(rows_pieces)
    unit, row_unit = pieces_unit(gate_pieces), pieces_unit(rows_pieces)

    def body(firsts_ref, *refs):
        out_ref, gate_ref, up_ref, second_ref = refs[-4:]

        @pl.when(pl.program_id(0) == 0)
        def _():
            join([firsts_ref[count + i] for i in range(parts)], refs[:parts], second_ref, row_unit)

        where = [firsts_ref[i] for i in range(count)]
        join(where, refs[parts : parts + count], gate_ref, unit)
        join(where, refs[parts + count : -4], up_ref, unit)
        second = second_ref[...]
        gate_sum = jnp.dot(second, gate_ref[...], preferred_element_type=jnp.float32)
        up_sum = jnp.dot(second, up_ref[...], preferred_element_type=jnp.float32)
        out_ref[...] = (gate_sum / (1.0 + jnp.exp(-gate_sum)) * up_sum).astype(jnp.bfloat16)

    return pl.pallas_call(
        body,
        grid=(pl.cdiv(units, tile),),
        in_specs=[pl.BlockSpec(memory_space=pltpu.SMEM)]
        + [pl.BlockSpec(h.shape, lambda i: (0, 0)) for h in rows_pieces]
        + [pl.BlockSpec((p.shape[0], tile), lambda i: (0, i)) for p in gate_pieces + up_pieces],
        out_specs=pl.BlockSpec((rows, tile), lambda i: (0, i)),
        out_shape=jax.ShapeDtypeStruct((rows, units), jnp.bfloat16),
        scratch_shapes=[
            pltpu.VMEM((depth, tile), jnp.bfloat16),
            pltpu.VMEM((depth, tile), jnp.bfloat16),
            pltpu.VMEM((rows, depth), jnp.bfloat16),
        ],
    )(jnp.stack(firsts + row_firsts).astype(jnp.int32), *rows_pieces, *gate_pieces, *up_pieces)


def blank_body(out_ref):
    pass


def blank(shape, dtype):
    return pl.pallas_call(
        blank_body,
        out_specs=pl.BlockSpec(memory_space=pl.ANY),
        out_shape=jax.ShapeDtypeStruct(shape, dtype),
        name="blank",
    )()


def core_swap(value):
    size = lax.axis_size("tp")
    return lax.ppermute(value, "tp", [(i, i ^ 1) for i in range(size)])


def chip_swap(value):
    size = lax.axis_size("tp")
    return lax.ppermute(value, "tp", [(i, (i + CORES) % size) for i in range(size)])


def small_tp():
    return lax.axis_size("tp") == 2 * CORES


def share_rows(rows):
    if small_tp():
        share = rows // CORES
        return (lax.axis_index("tp") % CORES) * share, share
    share = rows // lax.axis_size("tp")
    return lax.axis_index("tp") * share, share


def sum_groups(part):
    if not small_tp():
        return lax.psum_scatter(part, "tp", scatter_dimension=0, tiled=True).astype(jnp.float32)
    first, share = share_rows(part.shape[0])
    kept = lax.dynamic_slice_in_dim(part, first, share, 0)
    given = lax.dynamic_slice_in_dim(part, share - first, share, 0)
    chip = kept.astype(jnp.float32) + core_swap(given).astype(jnp.float32)
    chip = lax.reduce_precision(chip, 8, 7).astype(jnp.bfloat16)
    chip = lax.optimization_barrier(chip)
    return chip.astype(jnp.float32) + chip_swap(chip).astype(jnp.float32)


def collect_rows(value):
    if not small_tp():
        return [lax.all_gather(value, "tp", axis=0, tiled=True)], [jnp.int32(0)]
    share = value.shape[0]
    first = (lax.axis_index("tp") % CORES) * share
    return [value, core_swap(value)], [first, share - first]


def shards(
    layer_input_tokens,
    attention_norm_gain,
    query_projection,
    key_projection,
    value_projection,
    decay_first_factor,
    decay_second_factor,
    decay_logit_bias,
    extra_log_decay,
    head_output_gain,
    attention_output_projection,
    feedforward_norm_gain,
    gate_projection,
    up_projection,
    down_projection,
):
    rows = layer_input_tokens.shape[0]
    wide = jnp.float32
    local_heads = extra_log_decay.shape[1]
    width = query_projection.shape[1] // local_heads

    normed = norm_rows(layer_input_tokens, attention_norm_gain).astype(jnp.bfloat16)
    lowrank = jnp.dot(normed, decay_first_factor, preferred_element_type=wide).astype(jnp.bfloat16)
    logits = jnp.dot(lowrank, decay_second_factor, preferred_element_type=wide) + decay_logit_bias
    decays = jax.nn.log_sigmoid(logits) / DECAY_DIVISOR + jnp.repeat(extra_log_decay, width, axis=1)

    out_pieces = gather_rows([attention_output_projection])
    packed_pieces = gather_rows([query_projection, key_projection, value_projection], early=decays)
    gates = [gather_rows([gate_projection[:, a:b]]) for a, b in spans(gate_projection, GATE_CUTS)]
    ups = [gather_rows([up_projection[:, a:b]]) for a, b in spans(up_projection, GATE_CUTS)]
    down_spans = spans(down_projection, DOWN_CUTS)
    downs = [gather_rows([down_projection[:, a:b]], alone=i in ALONE) for i, (a, b) in enumerate(down_spans)]

    projected = dot_pieces([normed], packed_pieces)
    headed = attention(projected, decays, head_output_gain, local_heads)
    mixer = sum_groups(dot_pieces([headed], out_pieces, 512))

    first, share = share_rows(rows)
    own = lax.dynamic_slice_in_dim(layer_input_tokens, first, share, 0)
    residual = (own.astype(wide) + mixer).astype(jnp.bfloat16)
    second = collect_rows(norm_rows(residual, feedforward_norm_gain).astype(jnp.bfloat16))

    hidden = [gated(second, gates[i], ups[i]) for i in range(len(gates))]
    result = blank(layer_input_tokens.shape, jnp.bfloat16)
    for chunk, (start, stop) in enumerate(down_spans):
        channel = sum_groups(dot_pieces(hidden, downs[chunk]))
        finished = (residual[:, start:stop].astype(wide) + channel).astype(jnp.bfloat16)
        for piece, at in zip(*collect_rows(finished)):
            result = lax.dynamic_update_slice(result, piece, (at, jnp.int32(start)))
    return result


def spans(weight, cuts):
    width = weight.shape[1]
    edges = [0] + [round(width * cut / 128) * 128 for cut in cuts] + [width]
    return list(zip(edges, edges[1:]))


def solution(mesh):
    placed = (
        P(("grp", "fs"), None),
        P(),
        P("fs", "tp"),
        P("fs", "tp"),
        P("fs", "tp"),
        P(),
        P(None, "tp"),
        P("tp"),
        P(("grp", "fs"), "tp"),
        P(),
        P(("tp", "fs"), None),
        P(),
        P("fs", "tp"),
        P("fs", "tp"),
        P(("tp", "fs"), None),
    )

    return jax.shard_map(shards, mesh=mesh, in_specs=placed, out_specs=P(("grp", "fs"), None), check_vma=False)
```

```python
import jax
import jax.numpy as jnp
from jax import lax
from jax.experimental import pallas as pl
from jax.experimental.pallas import tpu as pltpu
from jax.sharding import PartitionSpec as P


BLOCK = 64
DOWN_CUTS = (0.5, 0.75)
ALONE = (1, 2)
DOWN_ORDER = (1, 0, 2)
DECAY_DIVISOR = 16.0
CORES = 2


def norm_rows(values, gain):
    wide = values.astype(jnp.float32)
    scale = lax.rsqrt(jnp.mean(wide * wide, axis=-1, keepdims=True) + 1e-06)
    return wide * scale * gain


def attention_body(query_ref, key_ref, value_ref, decay_ref, gain_ref, out_ref, acc_ref, ends_ref, fresh_ref, entry_ref):
    length, width = query_ref.shape
    value_width = value_ref.shape[1]
    count = length // BLOCK
    row = lax.broadcasted_iota(jnp.int32, (BLOCK, BLOCK), 0)
    col = lax.broadcasted_iota(jnp.int32, (BLOCK, BLOCK), 1)
    lower, upper = row >= col, row <= col
    sums = jnp.concatenate([lower.astype(jnp.float32), upper.astype(jnp.float32)], axis=0)
    half = BLOCK // 2
    nt = (((1,), (1,)), ((), ()))
    tn = (((0,), (0,)), ((), ()))

    for block in range(count):
        rows = pl.ds(block * BLOCK, BLOCK)
        decay = decay_ref[rows, :]
        both = jnp.dot(sums, decay, precision=lax.Precision.HIGHEST, preferred_element_type=jnp.float32)
        query = query_ref[rows, :].astype(jnp.float32)
        key = key_ref[rows, :].astype(jnp.float32)
        value = value_ref[rows, :]
        scores = None
        carried = []
        outgoing = []
        for running, middle_at, closing_at, mask in (
            (both[:BLOCK], half - 1, BLOCK - 1, lower),
            (both[BLOCK:], half, 0, upper),
        ):
            middle = running[middle_at : middle_at + 1]
            closing = running[closing_at : closing_at + 1]
            left = (query * jnp.exp(running - middle)).astype(jnp.bfloat16)
            right = (key * jnp.exp(middle - running)).astype(jnp.bfloat16)
            part = lax.dot_general(left, right, nt, preferred_element_type=jnp.float32)
            part = jnp.where(mask, part, 0.0)
            scores = part if scores is None else scores + part
            carried.append((query * jnp.exp(running)).astype(jnp.bfloat16))
            outgoing.append((key * jnp.exp(closing - running)).astype(jnp.bfloat16))
            side = len(carried) - 1
            ends_ref[block, :, side * width : (side + 1) * width] = jnp.exp(closing)
        acc_ref[rows, :] = jnp.dot(scores.astype(jnp.bfloat16), value, preferred_element_type=jnp.float32)
        entry_ref[block, :BLOCK, :] = jnp.concatenate(carried, axis=1)
        fresh_ref[block] = lax.dot_general(
            value, jnp.concatenate(outgoing, axis=1), tn, preferred_element_type=jnp.float32
        )

    state = [jnp.zeros((value_width, width), jnp.float32) for _ in range(2)]
    for step in range(count):
        for side, block in ((0, step), (1, count - 1 - step)):
            lanes = slice(side * width, (side + 1) * width)
            entry_ref[block, BLOCK:, lanes] = state[side].astype(jnp.bfloat16)
            state[side] = state[side] * ends_ref[block, :, lanes] + fresh_ref[block, :, lanes]
    for block in range(count):
        rows = pl.ds(block * BLOCK, BLOCK)
        mixed = acc_ref[rows, :] + lax.dot_general(
            entry_ref[block, :BLOCK, :], entry_ref[block, BLOCK:, :], nt, preferred_element_type=jnp.float32
        )
        scale = lax.rsqrt(jnp.mean(mixed * mixed, axis=-1, keepdims=True) + 1e-06)
        out_ref[rows, :] = (mixed * scale * gain_ref[...]).astype(jnp.bfloat16)


def attention(projected, decays, gain, heads):
    length = projected.shape[0]
    width = decays.shape[1] // heads
    value_width = gain.shape[0]
    count = length // BLOCK
    value_first = 2 * heads * width // value_width
    return pl.pallas_call(
        attention_body,
        grid=(heads,),
        in_specs=[
            pl.BlockSpec((length, width), lambda h: (0, h)),
            pl.BlockSpec((length, width), lambda h: (0, heads + h)),
            pl.BlockSpec((length, value_width), lambda h: (0, value_first + h)),
            pl.BlockSpec((length, width), lambda h: (0, h)),
            pl.BlockSpec((1, value_width), lambda h: (0, 0)),
        ],
        out_specs=pl.BlockSpec((length, value_width), lambda h: (0, h)),
        out_shape=jax.ShapeDtypeStruct((length, heads * value_width), jnp.bfloat16),
        scratch_shapes=[
            pltpu.VMEM((length, value_width), jnp.float32),
            pltpu.VMEM((count, 1, 2 * width), jnp.float32),
            pltpu.VMEM((count, value_width, 2 * width), jnp.float32),
            pltpu.VMEM((count, BLOCK + value_width, 2 * width), jnp.bfloat16),
        ],
        name="attention",
    )(projected, projected, projected, decays, gain.reshape(1, -1))


def gather_columns(parts):
    return parts[0] if len(parts) == 1 else jnp.concatenate(parts, axis=1)


def by_permutes(shape, rows):
    return shape["fs"] == 4 and shape["grp"] == 2 and rows % 32 == 0


def gather_rows(parts, alone=False, early=None):
    fs, grp = lax.axis_size("fs"), lax.axis_size("grp")
    rows = parts[0].shape[0]
    if not by_permutes({"fs": fs, "grp": grp}, rows):
        return [lax.all_gather(gather_columns(parts), "fs", axis=0, tiled=True)], [jnp.int32(0)]
    here, part = lax.axis_index("fs"), lax.axis_index("grp")
    shard = gather_columns(parts)
    half = rows if alone else rows // 2
    mine = shard
    if not alone:
        mine = gather_columns([lax.dynamic_slice_in_dim(p, part * half, half, 0) for p in parts])

    def shift(value, by):
        return lax.ppermute(value, "fs", [(i, (i + by) % fs) for i in range(fs)])

    def swap(value):
        return lax.ppermute(value, "grp", [(0, 1), (1, 0)])

    ahead = shift(mine, 1)
    behind = shift(mine, fs - 1)
    far = shift(ahead, 1)
    if early is not None:
        far = lax.optimization_barrier((far, early))[0]
    pieces, firsts = [shard], [here * rows]
    for piece, by in ((ahead, 1), (behind, fs - 1), (far, 2)):
        base = ((here + fs - by) % fs) * rows
        if alone:
            pieces.append(piece)
            firsts.append(base)
        else:
            pieces += [piece, swap(piece)]
            firsts += [base + part * half, base + (1 - part) * half]
    return pieces, firsts


def join(firsts, refs, full_ref, unit):
    for index, ref in enumerate(refs):
        first = pl.multiple_of(firsts[index], unit)
        full_ref[pl.ds(first, ref.shape[0]), :] = ref[...]


def pieces_unit(pieces):
    unit = 1
    while all(p.shape[0] % (2 * unit) == 0 for p in pieces):
        unit *= 2
    return unit


def dot_pieces(left, gathered, tile=256, first=None, halves=False):
    pieces, firsts = gathered
    (rows, depth), columns = left.shape, pieces[0].shape[1]
    tile = min(tile, columns)
    unit, count = pieces_unit(pieces), len(pieces)
    parts = CORES if halves else 1
    share = rows // parts
    moved = first is not None

    def body(firsts_ref, left_ref, *refs):
        outs = refs[count : count + parts]
        full_ref = refs[count + parts]
        if moved:
            ordered_ref = refs[-1]

            @pl.when(pl.program_id(0) == 0)
            def _():
                start = pl.multiple_of(firsts_ref[count], share)
                ordered_ref[:share, :] = left_ref[pl.ds(start, share), :]
                ordered_ref[share:, :] = left_ref[pl.ds(pl.multiple_of(share - start, share), share), :]

        else:
            ordered_ref = left_ref
        join([firsts_ref[i] for i in range(count)], refs[:count], full_ref, unit)
        product = jnp.dot(ordered_ref[...], full_ref[...], preferred_element_type=jnp.float32).astype(jnp.bfloat16)
        for part, out_ref in enumerate(outs):
            out_ref[...] = product[part * share : (part + 1) * share]

    out = pl.pallas_call(
        body,
        grid=(pl.cdiv(columns, tile),),
        in_specs=[pl.BlockSpec(memory_space=pltpu.SMEM), pl.BlockSpec(left.shape, lambda i: (0, 0))]
        + [pl.BlockSpec((p.shape[0], tile), lambda i: (0, i)) for p in pieces],
        out_specs=[pl.BlockSpec((share, tile), lambda i: (0, i))] * parts,
        out_shape=[jax.ShapeDtypeStruct((share, columns), jnp.bfloat16)] * parts,
        scratch_shapes=[pltpu.VMEM((depth, tile), jnp.bfloat16)]
        + ([pltpu.VMEM((rows, depth), jnp.bfloat16)] if moved else []),
    )(jnp.stack(firsts + ([first] if moved else [])).astype(jnp.int32), left, *pieces)
    return out if halves else out[0]


def gated(parts, gate, up, tile=256):
    (gate_pieces, firsts), up_pieces = gate, up[0]
    rows, (depth, units) = sum(p.shape[0] for p in parts), (parts[0].shape[1], gate_pieces[0].shape[1])
    unit, count = pieces_unit(gate_pieces), len(gate_pieces)

    def body(firsts_ref, *refs):
        out_ref, gate_ref, up_ref, rows_ref = refs[-4:]
        weights = refs[len(parts) : -4]

        @pl.when(pl.program_id(0) == 0)
        def _():
            at = 0
            for ref in refs[: len(parts)]:
                rows_ref[at : at + ref.shape[0], :] = ref[...]
                at += ref.shape[0]

        where = [firsts_ref[i] for i in range(count)]
        join(where, weights[:count], gate_ref, unit)
        join(where, weights[count:], up_ref, unit)
        second = rows_ref[...]
        gate_sum = jnp.dot(second, gate_ref[...], preferred_element_type=jnp.float32)
        up_sum = jnp.dot(second, up_ref[...], preferred_element_type=jnp.float32)
        out_ref[...] = (gate_sum / (1.0 + jnp.exp(-gate_sum)) * up_sum).astype(jnp.bfloat16)

    return pl.pallas_call(
        body,
        grid=(pl.cdiv(units, tile),),
        in_specs=[pl.BlockSpec(memory_space=pltpu.SMEM)]
        + [pl.BlockSpec(p.shape, lambda i: (0, 0)) for p in parts]
        + [pl.BlockSpec((p.shape[0], tile), lambda i: (0, i)) for p in gate_pieces + up_pieces],
        out_specs=pl.BlockSpec((rows, tile), lambda i: (0, i)),
        out_shape=jax.ShapeDtypeStruct((rows, units), jnp.bfloat16),
        scratch_shapes=[
            pltpu.VMEM((depth, tile), jnp.bfloat16),
            pltpu.VMEM((depth, tile), jnp.bfloat16),
            pltpu.VMEM((rows, depth), jnp.bfloat16),
        ],
    )(jnp.stack(firsts).astype(jnp.int32), *parts, *gate_pieces, *up_pieces)


def blank_body(out_ref):
    pass


def blank(shape, dtype):
    return pl.pallas_call(
        blank_body,
        out_specs=pl.BlockSpec(memory_space=pl.ANY),
        out_shape=jax.ShapeDtypeStruct(shape, dtype),
        name="blank",
    )()


def core_swap(value):
    size = lax.axis_size("tp")
    return lax.ppermute(value, "tp", [(i, i ^ 1) for i in range(size)])


def chip_swap(value):
    size = lax.axis_size("tp")
    return lax.ppermute(value, "tp", [(i, (i + CORES) % size) for i in range(size)])


def small_tp():
    return lax.axis_size("tp") == 2 * CORES


def share_rows(rows):
    if small_tp():
        share = rows // CORES
        return (lax.axis_index("tp") % CORES) * share, share
    share = rows // lax.axis_size("tp")
    return lax.axis_index("tp") * share, share


def sum_groups(parts):
    if not small_tp():
        return lax.psum_scatter(parts[0], "tp", scatter_dimension=0, tiled=True).astype(jnp.float32)
    kept, given = parts
    chip = kept.astype(jnp.float32) + core_swap(given).astype(jnp.float32)
    chip = lax.reduce_precision(chip, 8, 7).astype(jnp.bfloat16)
    chip = lax.optimization_barrier(chip)
    return chip.astype(jnp.float32) + chip_swap(chip).astype(jnp.float32)


def collect_rows(value):
    if not small_tp():
        return [lax.all_gather(value, "tp", axis=0, tiled=True)], [jnp.int32(0)]
    share = value.shape[0]
    first = (lax.axis_index("tp") % CORES) * share
    return [value, core_swap(value)], [first, share - first]


def shards(
    layer_input_tokens,
    attention_norm_gain,
    query_projection,
    key_projection,
    value_projection,
    decay_first_factor,
    decay_second_factor,
    decay_logit_bias,
    extra_log_decay,
    head_output_gain,
    attention_output_projection,
    feedforward_norm_gain,
    gate_projection,
    up_projection,
    down_projection,
):
    rows = layer_input_tokens.shape[0]
    wide = jnp.float32
    local_heads = extra_log_decay.shape[1]
    width = query_projection.shape[1] // local_heads

    normed = norm_rows(layer_input_tokens, attention_norm_gain).astype(jnp.bfloat16)
    lowrank = jnp.dot(normed, decay_first_factor, preferred_element_type=wide).astype(jnp.bfloat16)
    logits = jnp.dot(lowrank, decay_second_factor, preferred_element_type=wide) + decay_logit_bias
    decays = jax.nn.log_sigmoid(logits) / DECAY_DIVISOR + jnp.repeat(extra_log_decay, width, axis=1)

    out_pieces = gather_rows([attention_output_projection])
    packed_pieces = gather_rows([query_projection, key_projection, value_projection], early=decays)
    gate_pieces = gather_rows([gate_projection])
    up_pieces = gather_rows([up_projection])
    down_spans = spans(down_projection, DOWN_CUTS)
    downs = [gather_rows([down_projection[:, a:b]], alone=i in ALONE) for i, (a, b) in enumerate(down_spans)]

    projected = dot_pieces(normed, packed_pieces)
    headed = attention(projected, decays, head_output_gain, local_heads)
    first, share = share_rows(rows)
    halves = small_tp()
    mixed = dot_pieces(headed, out_pieces, 512, first if halves else None, halves)
    mixer = sum_groups(mixed if halves else [mixed])

    own = lax.dynamic_slice_in_dim(layer_input_tokens, first, share, 0)
    residual = (own.astype(wide) + mixer).astype(jnp.bfloat16)
    second, _ = collect_rows(norm_rows(residual, feedforward_norm_gain).astype(jnp.bfloat16))

    hidden = gated(second, gate_pieces, up_pieces)
    result = blank(layer_input_tokens.shape, jnp.bfloat16)
    for chunk in DOWN_ORDER:
        start, stop = down_spans[chunk]
        part = dot_pieces(hidden, downs[chunk], halves=halves)
        channel = sum_groups(part if halves else [part])
        finished = (residual[:, start:stop].astype(wide) + channel).astype(jnp.bfloat16)
        for piece, at in zip(*collect_rows(finished)):
            result = lax.dynamic_update_slice(result, piece, (at, jnp.int32(start)))
    return result


def spans(weight, cuts):
    width = weight.shape[1]
    edges = [0] + [round(width * cut / 128) * 128 for cut in cuts] + [width]
    return list(zip(edges, edges[1:]))


def solution(mesh):
    placed = (
        P(("grp", "fs"), None),
        P(),
        P("fs", "tp"),
        P("fs", "tp"),
        P("fs", "tp"),
        P(),
        P(None, "tp"),
        P("tp"),
        P(("grp", "fs"), "tp"),
        P(),
        P(("tp", "fs"), None),
        P(),
        P("fs", "tp"),
        P("fs", "tp"),
        P(("tp", "fs"), None),
    )

    return jax.shard_map(shards, mesh=mesh, in_specs=placed, out_specs=P(("grp", "fs"), None), check_vma=False)
```

```python
import jax
import jax.numpy as jnp
from jax import lax
from jax.experimental import pallas as pl
from jax.experimental.pallas import tpu as pltpu
from jax.sharding import PartitionSpec as P


BLOCK = 64
DOWN_CUTS = (0.5625, 0.6875)
ALONE = (1, 2)
DOWN_ORDER = (1, 0, 2)
GATE_CUTS = (0.55,)
TILE = 256
DECAY_DIVISOR = 16.0
CORES = 2


def norm_rows(values, gain):
    wide = values.astype(jnp.float32)
    scale = lax.rsqrt(jnp.mean(wide * wide, axis=-1, keepdims=True) + 1e-06)
    return wide * scale * gain


def attention_body(query_ref, key_ref, value_ref, decay_ref, gain_ref, out_ref, acc_ref, ends_ref, fresh_ref, entry_ref):
    length, width = query_ref.shape
    value_width = value_ref.shape[1]
    count = length // BLOCK
    row = lax.broadcasted_iota(jnp.int32, (BLOCK, BLOCK), 0)
    col = lax.broadcasted_iota(jnp.int32, (BLOCK, BLOCK), 1)
    lower, upper = row >= col, row <= col
    sums = jnp.concatenate([lower.astype(jnp.float32), upper.astype(jnp.float32)], axis=0)
    half = BLOCK // 2
    nt = (((1,), (1,)), ((), ()))
    tn = (((0,), (0,)), ((), ()))

    for block in range(count):
        rows = pl.ds(block * BLOCK, BLOCK)
        decay = decay_ref[rows, :]
        both = jnp.dot(sums, decay, precision=lax.Precision.HIGHEST, preferred_element_type=jnp.float32)
        query = query_ref[rows, :].astype(jnp.float32)
        key = key_ref[rows, :].astype(jnp.float32)
        value = value_ref[rows, :]
        scores = None
        carried = []
        outgoing = []
        for running, middle_at, closing_at, mask in (
            (both[:BLOCK], half - 1, BLOCK - 1, lower),
            (both[BLOCK:], half, 0, upper),
        ):
            middle = running[middle_at : middle_at + 1]
            closing = running[closing_at : closing_at + 1]
            left = (query * jnp.exp(running - middle)).astype(jnp.bfloat16)
            right = (key * jnp.exp(middle - running)).astype(jnp.bfloat16)
            part = lax.dot_general(left, right, nt, preferred_element_type=jnp.float32)
            part = jnp.where(mask, part, 0.0)
            scores = part if scores is None else scores + part
            carried.append((query * jnp.exp(running)).astype(jnp.bfloat16))
            outgoing.append((key * jnp.exp(closing - running)).astype(jnp.bfloat16))
            side = len(carried) - 1
            ends_ref[block, :, side * width : (side + 1) * width] = jnp.exp(closing)
        acc_ref[rows, :] = jnp.dot(scores.astype(jnp.bfloat16), value, preferred_element_type=jnp.float32)
        entry_ref[block, :BLOCK, :] = jnp.concatenate(carried, axis=1)
        fresh_ref[block] = lax.dot_general(
            value, jnp.concatenate(outgoing, axis=1), tn, preferred_element_type=jnp.float32
        )

    state = [jnp.zeros((value_width, width), jnp.float32) for _ in range(2)]
    for step in range(count):
        for side, block in ((0, step), (1, count - 1 - step)):
            lanes = slice(side * width, (side + 1) * width)
            entry_ref[block, BLOCK:, lanes] = state[side].astype(jnp.bfloat16)
            state[side] = state[side] * ends_ref[block, :, lanes] + fresh_ref[block, :, lanes]
    for block in range(count):
        rows = pl.ds(block * BLOCK, BLOCK)
        mixed = acc_ref[rows, :] + lax.dot_general(
            entry_ref[block, :BLOCK, :], entry_ref[block, BLOCK:, :], nt, preferred_element_type=jnp.float32
        )
        scale = lax.rsqrt(jnp.mean(mixed * mixed, axis=-1, keepdims=True) + 1e-06)
        out_ref[rows, :] = (mixed * scale * gain_ref[...]).astype(jnp.bfloat16)


def attention(projected, decays, gain, heads):
    length = projected.shape[0]
    width = decays.shape[1] // heads
    value_width = gain.shape[0]
    count = length // BLOCK
    value_first = 2 * heads * width // value_width
    return pl.pallas_call(
        attention_body,
        grid=(heads,),
        in_specs=[
            pl.BlockSpec((length, width), lambda h: (0, h)),
            pl.BlockSpec((length, width), lambda h: (0, heads + h)),
            pl.BlockSpec((length, value_width), lambda h: (0, value_first + h)),
            pl.BlockSpec((length, width), lambda h: (0, h)),
            pl.BlockSpec((1, value_width), lambda h: (0, 0)),
        ],
        out_specs=pl.BlockSpec((length, value_width), lambda h: (0, h)),
        out_shape=jax.ShapeDtypeStruct((length, heads * value_width), jnp.bfloat16),
        scratch_shapes=[
            pltpu.VMEM((length, value_width), jnp.float32),
            pltpu.VMEM((count, 1, 2 * width), jnp.float32),
            pltpu.VMEM((count, value_width, 2 * width), jnp.float32),
            pltpu.VMEM((count, BLOCK + value_width, 2 * width), jnp.bfloat16),
        ],
        name="attention",
    )(projected, projected, projected, decays, gain.reshape(1, -1))


def gather_columns(parts):
    return parts[0] if len(parts) == 1 else jnp.concatenate(parts, axis=1)


def by_permutes(shape, rows):
    return shape["fs"] == 4 and shape["grp"] == 2 and rows % 32 == 0


def gather_rows(parts, span=None, alone=False, early=None):
    fs, grp = lax.axis_size("fs"), lax.axis_size("grp")
    rows = parts[0].shape[0]
    whole = gather_columns(parts)
    start, stop = span or (0, whole.shape[1])
    shard = whole[:, start:stop]
    if not by_permutes({"fs": fs, "grp": grp}, rows):
        return [lax.all_gather(shard, "fs", axis=0, tiled=True)], [jnp.int32(0)], 0, stop - start
    here, part = lax.axis_index("fs"), lax.axis_index("grp")
    half = rows if alone else rows // 2
    mine = shard
    if not alone:
        mine = gather_columns([lax.dynamic_slice_in_dim(p, part * half, half, 0) for p in parts])[:, start:stop]

    def shift(value, by):
        return lax.ppermute(value, "fs", [(i, (i + by) % fs) for i in range(fs)])

    def swap(value):
        return lax.ppermute(value, "grp", [(0, 1), (1, 0)])

    ahead = shift(mine, 1)
    behind = shift(mine, fs - 1)
    far = shift(ahead, 1)
    if early is not None:
        far, _, whole = lax.optimization_barrier((far, early, whole))
    if start % TILE:
        whole, start = shard, 0
    pieces, firsts = [whole], [here * rows]
    for piece, by in ((ahead, 1), (behind, fs - 1), (far, 2)):
        base = ((here + fs - by) % fs) * rows
        if alone:
            pieces.append(piece)
            firsts.append(base)
        else:
            pieces += [piece, swap(piece)]
            firsts += [base + part * half, base + (1 - part) * half]
    return pieces, firsts, start, stop - (span or (0, 0))[0]


def join(firsts, refs, full_ref, unit):
    for index, ref in enumerate(refs):
        first = pl.multiple_of(firsts[index], unit)
        full_ref[pl.ds(first, ref.shape[0]), :] = ref[...]


def pieces_unit(pieces):
    unit = 1
    while all(p.shape[0] % (2 * unit) == 0 for p in pieces):
        unit *= 2
    return unit


def dot_pieces(left, gathered, tile=TILE, first=None, halves=False):
    pieces, firsts, offset, columns = gathered
    rows, depth = left.shape
    tile = min(tile, columns)
    unit, count = pieces_unit(pieces), len(pieces)
    parts = CORES if halves else 1
    share = rows // parts
    moved = first is not None

    def body(firsts_ref, left_ref, *refs):
        outs = refs[count : count + parts]
        full_ref = refs[count + parts]
        if moved:
            ordered_ref = refs[-1]

            @pl.when(pl.program_id(0) == 0)
            def _():
                start = pl.multiple_of(firsts_ref[count], share)
                ordered_ref[:share, :] = left_ref[pl.ds(start, share), :]
                ordered_ref[share:, :] = left_ref[pl.ds(pl.multiple_of(share - start, share), share), :]

        else:
            ordered_ref = left_ref
        join([firsts_ref[i] for i in range(count)], refs[:count], full_ref, unit)
        product = jnp.dot(ordered_ref[...], full_ref[...], preferred_element_type=jnp.float32).astype(jnp.bfloat16)
        for part, out_ref in enumerate(outs):
            out_ref[...] = product[part * share : (part + 1) * share]

    out = pl.pallas_call(
        body,
        grid=(pl.cdiv(columns, tile),),
        in_specs=[pl.BlockSpec(memory_space=pltpu.SMEM), pl.BlockSpec(left.shape, lambda i: (0, 0))]
        + [
            pl.BlockSpec((p.shape[0], tile), lambda i, skip=0 if n else offset // tile: (0, i + skip))
            for n, p in enumerate(pieces)
        ],
        out_specs=[pl.BlockSpec((share, tile), lambda i: (0, i))] * parts,
        out_shape=[jax.ShapeDtypeStruct((share, columns), jnp.bfloat16)] * parts,
        scratch_shapes=[pltpu.VMEM((depth, tile), jnp.bfloat16)]
        + ([pltpu.VMEM((rows, depth), jnp.bfloat16)] if moved else []),
    )(jnp.stack(firsts + ([first] if moved else [])).astype(jnp.int32), left, *pieces)
    return out if halves else out[0]


def gated(parts, gates, ups, tile=TILE):
    firsts = gates[0][1]
    count, unit = len(firsts), pieces_unit(gates[0][0])
    rows, depth = sum(p.shape[0] for p in parts), parts[0].shape[1]
    widths = [gate[3] for gate in gates]
    steps = [pl.cdiv(width, tile) for width in widths]
    starts = [sum(steps[:i]) for i in range(len(steps))]

    def body(firsts_ref, *refs):
        out_ref, gate_ref, up_ref, rows_ref = refs[-4:]
        weights = refs[len(parts) : -4]
        step = pl.program_id(0)

        @pl.when(step == 0)
        def _():
            at = 0
            for ref in refs[: len(parts)]:
                rows_ref[at : at + ref.shape[0], :] = ref[...]
                at += ref.shape[0]

        where = [firsts_ref[i] for i in range(count)]
        for group, (start, length) in enumerate(zip(starts, steps)):

            @pl.when(jnp.logical_and(step >= start, step < start + length))
            def _():
                at = 2 * group * count
                join(where, weights[at : at + count], gate_ref, unit)
                join(where, weights[at + count : at + 2 * count], up_ref, unit)

        second = rows_ref[...]
        gate_sum = jnp.dot(second, gate_ref[...], preferred_element_type=jnp.float32)
        up_sum = jnp.dot(second, up_ref[...], preferred_element_type=jnp.float32)
        out_ref[...] = (gate_sum / (1.0 + jnp.exp(-gate_sum)) * up_sum).astype(jnp.bfloat16)

    operands, specs = [], []
    for gate, up, start, length in zip(gates, ups, starts, steps):
        for number, piece in enumerate(gate[0] + up[0]):
            skip = 0 if number % count else gate[2] // tile

            def index(i, start=start, length=length, skip=skip):
                return 0, jnp.clip(i - start, 0, length - 1) + skip

            operands.append(piece)
            specs.append(pl.BlockSpec((piece.shape[0], tile), index))
    return pl.pallas_call(
        body,
        grid=(sum(steps),),
        in_specs=[pl.BlockSpec(memory_space=pltpu.SMEM)]
        + [pl.BlockSpec(p.shape, lambda i: (0, 0)) for p in parts]
        + specs,
        out_specs=pl.BlockSpec((rows, tile), lambda i: (0, i)),
        out_shape=jax.ShapeDtypeStruct((rows, sum(widths)), jnp.bfloat16),
        scratch_shapes=[
            pltpu.VMEM((depth, tile), jnp.bfloat16),
            pltpu.VMEM((depth, tile), jnp.bfloat16),
            pltpu.VMEM((rows, depth), jnp.bfloat16),
        ],
    )(jnp.stack(firsts).astype(jnp.int32), *parts, *operands)


def blank_body(out_ref):
    pass


def blank(shape, dtype):
    return pl.pallas_call(
        blank_body,
        out_specs=pl.BlockSpec(memory_space=pl.ANY),
        out_shape=jax.ShapeDtypeStruct(shape, dtype),
        name="blank",
    )()


def core_swap(value):
    size = lax.axis_size("tp")
    return lax.ppermute(value, "tp", [(i, i ^ 1) for i in range(size)])


def chip_swap(value):
    size = lax.axis_size("tp")
    return lax.ppermute(value, "tp", [(i, (i + CORES) % size) for i in range(size)])


def small_tp():
    return lax.axis_size("tp") == 2 * CORES


def share_rows(rows):
    if small_tp():
        share = rows // CORES
        return (lax.axis_index("tp") % CORES) * share, share
    share = rows // lax.axis_size("tp")
    return lax.axis_index("tp") * share, share


def sum_groups(parts):
    if not small_tp():
        return lax.psum_scatter(parts[0], "tp", scatter_dimension=0, tiled=True).astype(jnp.float32)
    kept, given = parts
    chip = kept.astype(jnp.float32) + core_swap(given).astype(jnp.float32)
    chip = lax.reduce_precision(chip, 8, 7).astype(jnp.bfloat16)
    chip = lax.optimization_barrier(chip)
    return chip.astype(jnp.float32) + chip_swap(chip).astype(jnp.float32)


def collect_rows(value):
    if not small_tp():
        return [lax.all_gather(value, "tp", axis=0, tiled=True)], [jnp.int32(0)]
    share = value.shape[0]
    first = (lax.axis_index("tp") % CORES) * share
    return [value, core_swap(value)], [first, share - first]


def shards(
    layer_input_tokens,
    attention_norm_gain,
    query_projection,
    key_projection,
    value_projection,
    decay_first_factor,
    decay_second_factor,
    decay_logit_bias,
    extra_log_decay,
    head_output_gain,
    attention_output_projection,
    feedforward_norm_gain,
    gate_projection,
    up_projection,
    down_projection,
):
    rows = layer_input_tokens.shape[0]
    wide = jnp.float32
    local_heads = extra_log_decay.shape[1]
    width = query_projection.shape[1] // local_heads

    normed = norm_rows(layer_input_tokens, attention_norm_gain).astype(jnp.bfloat16)
    lowrank = jnp.dot(normed, decay_first_factor, preferred_element_type=wide).astype(jnp.bfloat16)
    logits = jnp.dot(lowrank, decay_second_factor, preferred_element_type=wide) + decay_logit_bias
    decays = jax.nn.log_sigmoid(logits) / DECAY_DIVISOR + jnp.repeat(extra_log_decay, width, axis=1)

    out_pieces = gather_rows([attention_output_projection])
    packed_pieces = gather_rows([query_projection, key_projection, value_projection], early=decays)
    gate_spans = spans(gate_projection, GATE_CUTS, TILE)
    gates = [gather_rows([gate_projection], (a, b)) for a, b in gate_spans]
    ups = [gather_rows([up_projection], (a, b)) for a, b in gate_spans]
    down_spans = spans(down_projection, DOWN_CUTS)
    downs = [gather_rows([down_projection], (a, b), i in ALONE) for i, (a, b) in enumerate(down_spans)]

    projected = dot_pieces(normed, packed_pieces)
    headed = attention(projected, decays, head_output_gain, local_heads)
    first, share = share_rows(rows)
    halves = small_tp()
    mixed = dot_pieces(headed, out_pieces, 512, first if halves else None, halves)
    mixer = sum_groups(mixed if halves else [mixed])

    own = lax.dynamic_slice_in_dim(layer_input_tokens, first, share, 0)
    residual = (own.astype(wide) + mixer).astype(jnp.bfloat16)
    second, _ = collect_rows(norm_rows(residual, feedforward_norm_gain).astype(jnp.bfloat16))

    hidden = gated(second, gates, ups)
    result = blank(layer_input_tokens.shape, jnp.bfloat16)
    for chunk in DOWN_ORDER:
        start, stop = down_spans[chunk]
        part = dot_pieces(hidden, downs[chunk], downs[chunk][3], halves=halves)
        channel = sum_groups(part if halves else [part])
        finished = (residual[:, start:stop].astype(wide) + channel).astype(jnp.bfloat16)
        for piece, at in zip(*collect_rows(finished)):
            result = lax.dynamic_update_slice(result, piece, (at, jnp.int32(start)))
    return result


def spans(weight, cuts, tile=128):
    width = weight.shape[1]
    edges = [0] + [round(width * cut / tile) * tile for cut in cuts] + [width]
    return list(zip(edges, edges[1:]))


def solution(mesh):
    placed = (
        P(("grp", "fs"), None),
        P(),
        P("fs", "tp"),
        P("fs", "tp"),
        P("fs", "tp"),
        P(),
        P(None, "tp"),
        P("tp"),
        P(("grp", "fs"), "tp"),
        P(),
        P(("tp", "fs"), None),
        P(),
        P("fs", "tp"),
        P("fs", "tp"),
        P(("tp", "fs"), None),
    )

    return jax.shard_map(shards, mesh=mesh, in_specs=placed, out_specs=P(("grp", "fs"), None), check_vma=False)
```
